32 devices in a mesh: grp: 2 (over x), ep: 8 (over z, y), tp: 2 (over core).
Axes of the slice: x: 2, y: 2, z: 4, core: 2. Of those that a mesh axis runs over, the one named last changes fastest.
Arguments:
- tokens: bfloat16 [4096, 2048], P(('grp', 'ep', 'tp')), parts along dimension 0, may hold values from -6 to 6
- expert_ids: int32 [4096, 4], P(('grp', 'ep', 'tp')), parts along dimension 0, may hold values from 0 to 15, all different within a row; in each aligned block of 128 rows (0 to 127, 128 to 255, ...) at most 64 rows name the same one
- route_weights: float32 [4096, 4], P(('grp', 'ep', 'tp')), parts along dimension 0, may hold values from 0.05 to 1
- norm_gain: float32 [2048], replicated, may hold values from 0.1 to 1.9
- w_gate: bfloat16 [16, 2048, 896], P(('ep', 'tp')), may hold values from -0.5 to 0.5
- w_up: bfloat16 [16, 2048, 896], P(('ep', 'tp')), may hold values from -0.5 to 0.5
- w_down: bfloat16 [16, 896, 2048], P(('ep', 'tp')), may hold values from -0.0234375 to 0.0234375
Outputs:
- mixed: bfloat16 [4096, 2048], P(('grp', 'ep', 'tp')), parts along dimension 0
The draws below stay inside these ranges and needn't reach their ends.
There are 2 independent parts, one for each index of `grp`. The reference program is written for one: setup_inputs(seed, part) draws one part's arguments, and reference() takes and returns one part's arrays. A program takes and returns all parts, laid end to end along the dimension named above; an argument that names none is the same for every part. Nothing has to cross between parts.
Inputs may be any that keep to these rules, and one draw needn't show every extreme that they name: `expert_ids`: each token names 4 different experts. Among the 128 tokens of one device (aligned blocks of rows) no expert is named more than 64 times, a bound that some block reaches.
All inputs are finite; a program needn't handle non-finite values.
Results may differ from the reference program's by a relative error of at most 0.0071.
Values may be sent and summed in bfloat16 or wider, within the bound.
A program may use at most 64 MiB of HBM per device.

```python
import math
import jax
import jax.numpy as jnp
import numpy as np
from jax import lax

D = 2048
F = 896
TOPK = 4
TOK_DEV = 128
EXPERTS = 16
CAP = 64
TOKENS = 2048
N_EP = 8
N_TP = 2


def level_of(key, dims, cuts, smallest, high):
    factor_of = 1.0
    for dim, blocks in cuts:
        draws = jax.random.uniform(jax.random.fold_in(jax.random.fold_in(key, 6), dim), (blocks,), jnp.float32, smallest / len(cuts), high / len(cuts))
        factor_of = factor_of * jnp.repeat(jnp.exp(draws), dims[dim] // blocks).reshape((-1,) + (1,) * (len(dims) - 1 - dim))
    return factor_of


def shared_out(own_key, own, number, rows, amount, top, bound, slope):
    ranking = jax.random.permutation(own_key, amount)
    crowded, common = load_shares(amount, rows * top, bound, slope, True), load_shares(amount, rows * top, bound, slope, False)
    places = jnp.arange(amount)

    def named(sizes, turn):
        used = int((sizes > 0).sum())
        fixed = max(1, used // 4)
        shifted = fixed + (places - fixed + turn * (used - fixed)) % max(1, amount - fixed)
        return jnp.zeros((amount,), jnp.int32).at[ranking[jnp.where(places < fixed, places, shifted)]].set(jnp.asarray(sizes, jnp.int32))

    sizes = jnp.where(number % 4 == 0, named(crowded, number // 4), named(common, number - number // 4 - 1))
    mixed = jax.random.permutation(jax.random.fold_in(own, 3), amount)
    source_of, receiver = mixed[0:amount // 2 * 2:2], mixed[1:amount // 2 * 2:2]
    room = jnp.minimum(sizes[source_of] - 1, bound - sizes[receiver]) // 2
    room = jnp.where((source_of == ranking[0]) | (receiver == ranking[0]) | (sizes[receiver] == 0), 0, jnp.maximum(room, 0))
    shifted = jax.random.randint(jax.random.fold_in(own, 4), (amount // 2,), 0, 1 << 20) % (room + 1)
    sizes = sizes.at[source_of].add(-shifted).at[receiver].add(shifted)
    items = jnp.searchsorted(jnp.cumsum(sizes), jnp.arange(rows * top), side="right").astype(jnp.int32)
    grid = items.reshape(top, rows).T
    grid = grid[jax.random.permutation(jax.random.fold_in(own, 1), rows)]
    turn = jax.random.randint(jax.random.fold_in(own, 2), (rows, 1), 0, top)
    return jnp.take_along_axis(grid, (jnp.arange(top)[None, :] + turn) % top, axis=1)


def load_shares(amount, total, limit, lean, full):
    loads = [(1 << 20) // math.isqrt(standing ** lean) + 1 for standing in range(1, amount + 1)]
    largest = limit if full else min(limit, max(-(-total // amount), total * loads[0] // sum(loads)))
    least = 1 if total - largest >= amount - 1 else 0
    given, surplus = [largest] + [least] * (amount - 1), total - largest - least * (amount - 1)
    while surplus > 0:
        free = [i for i in range(1, amount) if given[i] < largest] or [i for i in range(1, amount) if given[i] < limit]
        whole, left = sum([loads[i] for i in free]), surplus
        for i in free:
            extra = min(limit - given[i], max(1, left * loads[i] // whole), surplus)
            given[i] = given[i] + extra
            surplus = surplus - extra
    return np.array(given)


def noise(stream_key, shape, scale, limit, cuts=(), kind=jnp.bfloat16):
    gain = level_of(stream_key, shape, cuts, -0.22, 0.18) if cuts else 1.0
    values = jax.random.normal(stream_key, shape, jnp.float32) * scale * gain
    return jnp.minimum(jnp.maximum(values, -limit), limit).astype(kind)


def setup_inputs(seed: int = 0, part: int = 0) -> dict:
    splits = jax.random.split(jax.random.key(seed), 8)
    part_splits = jax.random.split(jax.random.fold_in(splits[7], part), 8)
    tokens = noise(part_splits[0], (TOKENS, D), 1.0, 6.0, ((0, 16),))
    expert_ids_keys = jax.random.split(jax.random.fold_in(part_splits[1], 1), TOKENS // TOK_DEV)
    expert_ids_turns = jax.random.permutation(jax.random.fold_in(part_splits[1], 3), TOKENS // TOK_DEV)
    expert_ids = jax.vmap(lambda own, number: shared_out(jax.random.fold_in(part_splits[1], 2), own, number, TOK_DEV, EXPERTS, TOPK, CAP, 2))(expert_ids_keys, expert_ids_turns).reshape((TOKENS, TOPK))
    route_weights = jnp.clip(jnp.exp(math.log(1.0) - 2.9957323 * jax.random.uniform(part_splits[2], (TOKENS, TOPK), jnp.float32) ** level_of(part_splits[2], (TOKENS, TOPK), ((0, 16),), -0.2, 0.2)), 0.05, 1.0)
    norm_gain = jnp.clip(1.0 + 0.18 * jax.random.normal(splits[3], (D,), jnp.float32), 0.1, 1.9)
    w_gate = noise(splits[4], (EXPERTS, D, F), (D // 16) ** -0.5, 0.5, ((0, 16),))
    w_up = noise(splits[5], (EXPERTS, D, F), (D // 16) ** -0.5, 0.5, ((0, 16),))
    w_down = noise(splits[6], (EXPERTS, F, D), (64 * F) ** -0.5, 0.0234375, ((0, 16),))
    return {"tokens": tokens, "expert_ids": expert_ids, "route_weights": route_weights, "norm_gain": norm_gain, "w_gate": w_gate, "w_up": w_up, "w_down": w_down}


norm_eps = 1e-05
clamp_limit = 7.0
sig_alpha = 1.702

def layer_norm(tokens, norm_gain):
    values = tokens.astype(jnp.float32)
    row_mean = lax.optimization_barrier(jnp.mean(values, -1, keepdims=True))
    centred = values - row_mean
    row_var = lax.optimization_barrier(jnp.mean(centred * centred, -1, keepdims=True))
    scaled = centred * lax.rsqrt(row_var + norm_eps) * norm_gain.astype(jnp.float32)
    return scaled.astype(jnp.bfloat16)

def expert_apply(inputs, gate_mat, up_mat, down_mat):
    gate_pre = jnp.dot(inputs, gate_mat, preferred_element_type=jnp.float32)
    up_pre = jnp.dot(inputs, up_mat, preferred_element_type=jnp.float32)
    gated = jnp.minimum(gate_pre, clamp_limit)
    upper = jnp.clip(up_pre, -clamp_limit, clamp_limit)
    hidden = (gated * jax.nn.sigmoid(sig_alpha * gated) * (upper + 1.0)).astype(jnp.bfloat16)
    return jnp.dot(hidden, down_mat, preferred_element_type=jnp.float32).astype(jnp.bfloat16)

def reference(tokens, expert_ids, route_weights, norm_gain, w_gate, w_up, w_down):
    normed = layer_norm(tokens, norm_gain)
    flat_ids = expert_ids.reshape(-1).astype(jnp.int32)
    sorted_pairs = jnp.argsort(flat_ids, stable=True).astype(jnp.int32)
    counts = lax.optimization_barrier(jnp.sum((flat_ids[:, None] == jnp.arange(EXPERTS, dtype=jnp.int32)[None, :]).astype(jnp.int32), 0))
    starts = (jnp.cumsum(counts) - counts).astype(jnp.int32)
    slot_limit = N_EP * N_TP * CAP
    padded = jnp.concatenate([sorted_pairs, jnp.zeros((slot_limit,), jnp.int32)])
    pair_weights = route_weights.reshape(-1).astype(jnp.float32)

    def add_expert(accum_total, inputs):
        expert, gate_mat, up_mat, down_mat = inputs
        pair_index = lax.dynamic_slice_in_dim(padded, starts[expert].astype(jnp.int32), slot_limit)
        live_mask = jnp.arange(slot_limit, dtype=jnp.int32) < counts[expert]
        token_index = (pair_index // TOPK).astype(jnp.int32)
        results = expert_apply(normed[token_index], gate_mat, up_mat, down_mat)
        factor = jnp.where(live_mask, pair_weights[pair_index], jnp.zeros((), jnp.float32))
        scaled = factor[:, None] * results.astype(jnp.float32)
        return (accum_total.at[token_index].add(scaled), None)
    start_total = jnp.zeros((TOKENS, D), jnp.float32)
    accum_total, unused = lax.scan(add_expert, start_total, (jnp.arange(EXPERTS, dtype=jnp.int32), w_gate, w_up, w_down))
    return accum_total.astype(jnp.bfloat16)
```

```python
import jax
import jax.numpy as jnp
from jax import lax
from jax.sharding import PartitionSpec as P

norm_eps = 1e-05
clamp_limit = 7.0
sig_alpha = 1.702


def layer_norm(tokens, norm_gain):
    values = tokens.astype(jnp.float32)
    row_mean = jnp.mean(values, -1, keepdims=True)
    centred = values - row_mean
    row_var = jnp.mean(centred * centred, -1, keepdims=True)
    scaled = centred * lax.rsqrt(row_var + norm_eps) * norm_gain
    return scaled.astype(jnp.bfloat16)


def expert_apply(inputs, gate_mat, up_mat, down_mat):
    gate_pre = jnp.dot(inputs, gate_mat, preferred_element_type=jnp.float32)
    up_pre = jnp.dot(inputs, up_mat, preferred_element_type=jnp.float32)
    gated = jnp.minimum(gate_pre, clamp_limit)
    upper = jnp.clip(up_pre, -clamp_limit, clamp_limit)
    hidden = (gated * jax.nn.sigmoid(sig_alpha * gated) * (upper + 1.0)).astype(jnp.bfloat16)
    return jnp.dot(hidden, down_mat, preferred_element_type=jnp.float32).astype(jnp.bfloat16)


def local_exchange(tokens, expert_ids, route_weights, norm_gain, w_gate, w_up, w_down):
    ep_count = lax.axis_size("ep")
    tp_count = lax.axis_size("tp")
    experts = ep_count * tp_count
    tok_rows, feat_width = tokens.shape
    top_count = expert_ids.shape[1]
    capacity = 2 * tok_rows * top_count // experts
    normed = layer_norm(tokens, norm_gain)
    flat_ids = expert_ids.reshape(-1)
    one_hot = (flat_ids[:, None] == jnp.arange(experts, dtype=jnp.int32)[None, :]).astype(jnp.int32)
    slot_index = jnp.sum((jnp.cumsum(one_hot, 0) - one_hot) * one_hot, 1)
    target = flat_ids * capacity + slot_index
    pair_token = jnp.arange(tok_rows * top_count, dtype=jnp.int32) // top_count
    buffer = (
        jnp.zeros((experts * capacity, feat_width), jnp.bfloat16).at[target].set(normed[pair_token])
    )
    buffer = buffer.reshape(experts, capacity, feat_width)
    gate_mat = w_gate[0]
    up_mat = w_up[0]
    down_mat = w_down[0]
    arrived = lax.all_to_all(buffer, ("ep", "tp"), split_axis=0, concat_axis=0, tiled=True)
    flat_rows = arrived.reshape(-1, feat_width)
    returned = lax.all_to_all(
        expert_apply(flat_rows, gate_mat, up_mat, down_mat).reshape(arrived.shape),
        ("ep", "tp"),
        split_axis=0,
        concat_axis=0,
        tiled=True,
    )
    picked = returned.reshape(experts * capacity, feat_width)[target].reshape(
        tok_rows, top_count, feat_width
    )
    combined = jnp.zeros((tok_rows, feat_width), jnp.float32)
    for choice_slot in range(top_count):
        combined = combined + route_weights[:, choice_slot : choice_slot + 1] * picked[
            :, choice_slot
        ].astype(jnp.float32)
    return combined.astype(jnp.bfloat16)


def local_gather(tokens, expert_ids, route_weights, norm_gain, w_gate, w_up, w_down):
    axes = ("ep", "tp")
    experts = lax.axis_size("ep") * lax.axis_size("tp")
    normed = layer_norm(tokens, norm_gain)
    chosen = expert_ids[:, :, None] == jnp.arange(experts, dtype=jnp.int32)
    dense = jnp.sum(jnp.where(chosen, route_weights[:, :, None], 0.0), 1)
    factor = lax.all_to_all(dense, axes, split_axis=1, concat_axis=0, tiled=True)
    gathered = lax.all_gather(normed, axes, axis=0, tiled=True)
    results = expert_apply(gathered, w_gate[0], w_up[0], w_down[0])
    scaled = (factor * results.astype(jnp.float32)).astype(jnp.bfloat16)
    return lax.psum_scatter(scaled, axes, scatter_dimension=0, tiled=True)


def local(tokens, expert_ids, *rest):
    experts = lax.axis_size("ep") * lax.axis_size("tp")
    tok_rows, top_count = expert_ids.shape
    capacity = 2 * tok_rows * top_count // experts
    whole_blocks = lax.axis_size("tp") * capacity >= tok_rows
    return (local_gather if whole_blocks else local_exchange)(tokens, expert_ids, *rest)


def solution(mesh):
    placed = (
        P(("grp", "ep", "tp"), None),
        P(("grp", "ep", "tp"), None),
        P(("grp", "ep", "tp"), None),
        P(),
        P(("ep", "tp"), None, None),
        P(("ep", "tp"), None, None),
        P(("ep", "tp"), None, None),
    )
    return jax.shard_map(
        local, mesh=mesh, in_specs=placed, out_specs=P(("grp", "ep", "tp"), None), check_vma=False
    )
```
